32 devices in a mesh: sp: 8 (over z, x), tp: 4 (over y, core).
Axes of the slice: x: 2, y: 2, z: 4, core: 2. Of those that a mesh axis runs over, the one named last changes fastest.
Arguments:
- queries: bfloat16 [512, 16, 192], P('sp', 'tp'), may hold values from -400 to 400
- latents: bfloat16 [512, 512], P('sp'), may hold values from -6 to 6
- rope_keys: bfloat16 [512, 64], P('sp'), may hold values from -9 to 9
- latent_norm_scale: float32 [512], replicated, may hold values from 0.1 to 1.9
- key_value_weight: bfloat16 [512, 16, 256], P(None, 'tp'), may hold values from -0.25 to 0.25
- out_weight: bfloat16 [2048, 2048], P('tp'), may hold values from -1 to 1
- resid: bfloat16 [512, 2048], P('sp'), may hold values from -3 to 3
- ffn_gain: float32 [2048], replicated, may hold values from 0.1 to 1.9
- expert_ids: int32 [512, 2], P('sp'), may hold values from 0 to 7, all different within a row; in each aligned block of 64 rows (0 to 63, 64 to 127, ...) at most 24 rows name the same one
- route_weights: float32 [512, 2], P('sp'), may hold values from 0.1 to 1
- gate_weight: bfloat16 [8, 2048, 4096], P('sp', None, 'tp'), may hold values from -0.125 to 0.125
- up_weight: bfloat16 [8, 2048, 4096], P('sp', None, 'tp'), may hold values from -0.125 to 0.125
- down_weight: bfloat16 [8, 4096, 2048], P('sp', 'tp'), may hold values from -0.09375 to 0.09375
Outputs:
- updated: bfloat16 [512, 2048], P('sp', 'tp')
The draws below stay inside these ranges and needn't reach their ends.
Inputs may be any that keep to these rules, and one draw needn't show every extreme that they name: `expert_ids`: among the rows of one device no expert is named more than 24 times, and in some devices some expert is named exactly 24 times.
All inputs are finite; a program needn't handle non-finite values.
Results may differ from the reference program's by a relative error of at most 0.025.
Values may be sent and summed in bfloat16 or wider, within the bound.
No kernel may reach another device: no remote copies, remote signals or barrier semaphores. Data moves between devices by JAX's collectives and lax.ppermute only.
A program may use at most 64 MiB of HBM per device.

```python
import math
import jax
import jax.numpy as jnp
import numpy as np
from jax import lax

D = 2048
HEAD_COUNT = 16
PLAIN_WIDTH = 128
RD = 64
VALUE_WIDTH = 128
LATENT_WIDTH = 512
FF_E = 4096
TOP = 2
TOK_DEV = 64
TOKEN_COUNT = 512
EXPERTS = 8
CAP = 24
N_SP = 8
N_TP = 4


def drawn_base(key):
    keys_all = jnp.clip(jax.random.normal(jax.random.fold_in(key, 101), (TOKEN_COUNT, RD), jnp.float32), -6.0, 6.0)
    return keys_all


def draw_rope_keys(key, part):
    keys_all = drawn_base(key)
    return keys_all.astype(jnp.bfloat16)


def draw_queries(key, part):
    base = jnp.clip(1.5 * jax.random.normal(jax.random.fold_in(key, 103), (TOKEN_COUNT, HEAD_COUNT, PLAIN_WIDTH + RD), jnp.float32), -9.0, 9.0)
    return base.astype(jnp.bfloat16)


def level_of(stream_key, shape, split, least, largest):
    loudness, own = 1.0, jax.random.fold_in(stream_key, 6)
    for position, shards_of in split:
        steps = jnp.exp(jax.random.uniform(jax.random.fold_in(own, position), (shards_of,), jnp.float32, least / len(split), largest / len(split)))
        loudness = loudness * jnp.repeat(steps, shape[position] // shards_of).reshape([-1 if axis == position else 1 for axis in range(len(shape))])
    return loudness


def deal_out(own_key, own, number, rows, amount, top, reach, lean):
    ranking = jax.random.permutation(own_key, amount)
    heavy_load, ordinary = load_shares(amount, rows * top, reach, lean, True), load_shares(amount, rows * top, reach, lean, False)
    places = jnp.arange(amount)

    def named(tallies, turn):
        used = int((tallies > 0).sum())
        fixed = max(1, used // 4)
        moved = fixed + (places - fixed + turn * (used - fixed)) % max(1, amount - fixed)
        return jnp.zeros((amount,), jnp.int32).at[ranking[jnp.where(places < fixed, places, moved)]].set(jnp.asarray(tallies, jnp.int32))

    tallies = jnp.where(number % 4 == 0, named(heavy_load, number // 4), named(ordinary, number - number // 4 - 1))
    mixed = jax.random.permutation(jax.random.fold_in(own, 3), amount)
    source_of, receiver = mixed[0:amount // 2 * 2:2], mixed[1:amount // 2 * 2:2]
    slack = jnp.minimum(tallies[source_of] - 1, reach - tallies[receiver]) // 2
    slack = jnp.where((source_of == ranking[0]) | (receiver == ranking[0]) | (tallies[receiver] == 0), 0, jnp.maximum(slack, 0))
    moved = jax.random.randint(jax.random.fold_in(own, 4), (amount // 2,), 0, 1 << 20) % (slack + 1)
    tallies = tallies.at[source_of].add(-moved).at[receiver].add(moved)
    items = jnp.searchsorted(jnp.cumsum(tallies), jnp.arange(rows * top), side="right").astype(jnp.int32)
    table = items.reshape(top, rows).T
    table = table[jax.random.permutation(jax.random.fold_in(own, 1), rows)]
    turn = jax.random.randint(jax.random.fold_in(own, 2), (rows, 1), 0, top)
    return jnp.take_along_axis(table, (jnp.arange(top)[None, :] + turn) % top, axis=1)


def load_shares(number_of, total, limit, slope, full):
    loads = [(1 << 20) // math.isqrt(grade ** slope) + 1 for grade in range(1, number_of + 1)]
    largest = limit if full else min(limit, max(-(-total // number_of), total * loads[0] // sum(loads)))
    least = 1 if total - largest >= number_of - 1 else 0
    counts, rest = [largest] + [least] * (number_of - 1), total - largest - least * (number_of - 1)
    while rest > 0:
        free = [i for i in range(1, number_of) if counts[i] < largest] or [i for i in range(1, number_of) if counts[i] < limit]
        mass, remaining = sum([loads[i] for i in free]), rest
        for i in free:
            more = min(limit - counts[i], max(1, remaining * loads[i] // mass), rest)
            counts[i] = counts[i] + more
            rest = rest - more
    return np.array(counts)


def scatter_about(rng, shape, deviation, limit, cuts=(), held_as=jnp.bfloat16):
    result = jax.random.normal(rng, shape, jnp.float32) * deviation
    if len(cuts) > 0:
        result = level_of(rng, shape, cuts, -0.22, 0.18) * result
    return jnp.clip(result, min=-limit, max=limit).astype(held_as)


def setup_inputs(seed: int = 0) -> dict:
    keys = jax.random.split(jax.random.key(seed), 14)
    queries = draw_queries(jax.random.fold_in(keys[13], 71), 0)
    latents = scatter_about(keys[1], (TOKEN_COUNT, LATENT_WIDTH), 1.0, 6.0, ((0, 8),))
    rope_keys = draw_rope_keys(jax.random.fold_in(keys[13], 71), 0)
    latent_norm_scale = jnp.clip(1.0 + 0.18 * jax.random.normal(keys[3], (LATENT_WIDTH,), jnp.float32), 0.1, 1.9)
    key_value_weight = scatter_about(keys[4], (LATENT_WIDTH, HEAD_COUNT, PLAIN_WIDTH + VALUE_WIDTH), LATENT_WIDTH ** -0.5, 0.25, ((1, 4),))
    out_weight = scatter_about(keys[5], (HEAD_COUNT * VALUE_WIDTH, D), (HEAD_COUNT * VALUE_WIDTH // 64) ** -0.5, 1.0, ((0, 4),))
    resid = scatter_about(keys[6], (TOKEN_COUNT, D), 0.5, 3.0, ((0, 8),))
    ffn_gain = jnp.clip(1.0 + 0.18 * jax.random.normal(keys[7], (D,), jnp.float32), 0.1, 1.9)
    expert_ids_keys = jax.random.split(jax.random.fold_in(keys[8], 1), TOKEN_COUNT // TOK_DEV)
    expert_ids_turns = jax.random.permutation(jax.random.fold_in(keys[8], 3), TOKEN_COUNT // TOK_DEV)
    expert_ids = jax.vmap(lambda own, number: deal_out(jax.random.fold_in(keys[8], 2), own, number, TOK_DEV, EXPERTS, TOP, CAP, 2))(expert_ids_keys, expert_ids_turns).reshape((TOKEN_COUNT, TOP))
    route_weights = jnp.clip(0.1 + 0.9 * jax.random.uniform(keys[9], (TOKEN_COUNT, TOP), jnp.float32) ** level_of(keys[9], (TOKEN_COUNT, TOP), ((0, 8),), -0.2, 0.2), 0.1, 1.0)
    gate_weight = scatter_about(keys[10], (EXPERTS, D, FF_E), D ** -0.5, 0.125, ((0, 8), (2, 4)))
    up_weight = scatter_about(keys[11], (EXPERTS, D, FF_E), D ** -0.5, 0.125, ((0, 8), (2, 4)))
    down_weight = scatter_about(keys[12], (EXPERTS, FF_E, D), FF_E ** -0.5, 0.09375, ((0, 8), (1, 4)))
    return {"queries": queries, "latents": latents, "rope_keys": rope_keys, "latent_norm_scale": latent_norm_scale, "key_value_weight": key_value_weight, "out_weight": out_weight, "resid": resid, "ffn_gain": ffn_gain, "expert_ids": expert_ids, "route_weights": route_weights, "gate_weight": gate_weight, "up_weight": up_weight, "down_weight": down_weight}


rope_base = 10000.0
norm_eps = 1e-06

def rotary_table(positions, width):
    half_width = width // 2
    inverse = rope_base ** (-jnp.arange(half_width, dtype=jnp.float32) / half_width)
    turned = positions[:, None] * inverse[None, :]
    return (jnp.cos(turned), jnp.sin(turned))

def turn_pairs(vectors, cosines, sines):
    half_width = vectors.shape[-1] // 2
    front_half = vectors[..., :half_width]
    back_half = vectors[..., half_width:]
    return jnp.concatenate([front_half * cosines - back_half * sines, back_half * cosines + front_half * sines], axis=-1)

def rms_scaled(matrix, gain):
    floats = matrix.astype(jnp.float32)
    return floats * lax.rsqrt(lax.optimization_barrier(jnp.mean(floats * floats, axis=-1, keepdims=True)) + norm_eps) * gain

def reference(queries, latents, rope_keys, latent_norm_scale, key_value_weight, out_weight, resid, ffn_gain, expert_ids, route_weights, gate_weight, up_weight, down_weight):
    positions = jnp.arange(TOKEN_COUNT, dtype=jnp.float32)
    cosines, sines = rotary_table(positions, RD)
    normalized_latent = rms_scaled(latents, latent_norm_scale).astype(jnp.bfloat16)
    projected_rows = jnp.dot(normalized_latent, key_value_weight.reshape(LATENT_WIDTH, HEAD_COUNT * (PLAIN_WIDTH + VALUE_WIDTH)), preferred_element_type=jnp.float32)
    projected_rows = lax.optimization_barrier(projected_rows.astype(jnp.bfloat16)).astype(jnp.float32).reshape(TOKEN_COUNT, HEAD_COUNT, PLAIN_WIDTH + VALUE_WIDTH)
    key_plain = projected_rows[:, :, :PLAIN_WIDTH]
    head_values = projected_rows[:, :, PLAIN_WIDTH:]
    key_turned = turn_pairs(rope_keys.astype(jnp.float32), cosines, sines)
    key_turned = lax.optimization_barrier(key_turned.astype(jnp.bfloat16)).astype(jnp.float32)
    query_plain = queries[:, :, :PLAIN_WIDTH].astype(jnp.float32)
    query_turned = turn_pairs(queries[:, :, PLAIN_WIDTH:].astype(jnp.float32), cosines[:, None, :], sines[:, None, :])
    query_turned = lax.optimization_barrier(query_turned.astype(jnp.bfloat16)).astype(jnp.float32)
    score_scale = (PLAIN_WIDTH + RD) ** (-0.5)
    block_rows = math.gcd(TOKEN_COUNT, 256)
    block_count = TOKEN_COUNT // block_rows

    def attend_block(block_inputs):
        plain_block, turned_block = block_inputs
        scores = (jnp.einsum('qhn,khn->hqk', plain_block, key_plain) + jnp.einsum('qhr,kr->hqk', turned_block, key_turned)) * score_scale
        highest = lax.optimization_barrier(jnp.max(scores, axis=-1, keepdims=True))
        exps = jnp.exp(scores - highest)
        totals = lax.optimization_barrier(jnp.sum(exps, axis=-1))
        weights = lax.optimization_barrier(exps.astype(jnp.bfloat16)).astype(jnp.float32)
        summed = jnp.einsum('hqk,khv->qhv', weights, head_values)
        return (summed / jnp.transpose(totals)[:, :, None]).astype(jnp.bfloat16)
    attended = lax.map(attend_block, (query_plain.reshape(block_count, block_rows, HEAD_COUNT, PLAIN_WIDTH), query_turned.reshape(block_count, block_rows, HEAD_COUNT, RD)))
    attended = attended.reshape(TOKEN_COUNT, HEAD_COUNT * VALUE_WIDTH)
    mixed = jnp.dot(attended, out_weight, preferred_element_type=jnp.float32)
    middle = (resid.astype(jnp.float32) + mixed).astype(jnp.bfloat16)
    normed = rms_scaled(middle, ffn_gain).astype(jnp.bfloat16)
    expert_rows = N_SP * CAP
    flat_ids = expert_ids.reshape(-1).astype(jnp.int32)
    picked = (flat_ids[:, None] == jnp.arange(EXPERTS, dtype=jnp.int32)[None, :]).astype(jnp.int32)
    slot_rank = lax.optimization_barrier(jnp.sum((jnp.cumsum(picked, axis=0) - picked) * picked, axis=1)).astype(jnp.int32)
    slot_index = flat_ids * expert_rows + slot_rank
    sources = jnp.arange(TOKEN_COUNT * TOP, dtype=jnp.int32) // TOP
    owner_row = jnp.zeros((EXPERTS * expert_rows,), jnp.int32).at[slot_index].set(sources)
    filled = jnp.zeros((EXPERTS * expert_rows,), jnp.bool_).at[slot_index].set(True)

    def run_expert(expert_inputs):
        owners, present, gate_matrix, up_matrix, down_matrix = expert_inputs
        rows_in = jnp.where(present[:, None], normed[owners], jnp.zeros((), jnp.bfloat16))
        gate_act = jnp.dot(rows_in, gate_matrix, preferred_element_type=jnp.float32)
        up_act = jnp.dot(rows_in, up_matrix, preferred_element_type=jnp.float32)
        hidden = (jax.nn.silu(gate_act) * up_act).astype(jnp.bfloat16)
        partials = jnp.einsum('rbf,bfd->brd', hidden.astype(jnp.float32).reshape(expert_rows, N_TP, FF_E // N_TP), down_matrix.astype(jnp.float32).reshape(N_TP, FF_E // N_TP, D))
        rounded = lax.optimization_barrier(partials.astype(jnp.bfloat16)).astype(jnp.float32)
        return lax.optimization_barrier(jnp.sum(rounded, axis=0)).astype(jnp.bfloat16)
    outputs = lax.map(run_expert, (owner_row.reshape(EXPERTS, expert_rows), filled.reshape(EXPERTS, expert_rows), gate_weight, up_weight, down_weight))
    chosen_rows = outputs.reshape(EXPERTS * expert_rows, D)[slot_index].astype(jnp.float32) * route_weights.reshape(-1)[:, None]
    routed = lax.optimization_barrier(jnp.sum(chosen_rows.reshape(TOKEN_COUNT, TOP, D), axis=1))
    return (middle.astype(jnp.float32) + routed).astype(jnp.bfloat16)
```

```python
import jax
import jax.numpy as jnp
from jax import lax
from jax.sharding import PartitionSpec as P

PLAIN_WIDTH = 128
VALUE_WIDTH = 128

rope_base = 10000.0
norm_eps = 1e-06


f32 = jnp.float32
bf16 = jnp.bfloat16


def rotary_table(positions, width):
    half_width = width // 2
    inverse = rope_base ** (-jnp.arange(half_width, dtype=f32) / half_width)
    turned = positions[:, None] * inverse[None, :]
    return (jnp.cos(turned), jnp.sin(turned))


def turn_pairs(vectors, cosines, sines):
    half_width = vectors.shape[-1] // 2
    front_half = vectors[..., :half_width]
    back_half = vectors[..., half_width:]
    return jnp.concatenate(
        [front_half * cosines - back_half * sines, back_half * cosines + front_half * sines],
        axis=-1,
    )


def rms_scaled(matrix, gain):
    floats = matrix.astype(f32)
    return floats * lax.rsqrt(jnp.mean(floats * floats, axis=-1, keepdims=True) + norm_eps) * gain


def swap(value, axis, distance):
    count = lax.axis_size(axis)
    return lax.ppermute(value, axis, [(i, i ^ distance) for i in range(count)])


def core_halves(matrix, columns, core):
    blocks = [matrix[:, i : i + columns] for i in range(0, matrix.shape[1], columns)]
    mine = [jnp.where(core == 0, a, b) for a, b in zip(blocks[::2], blocks[1::2])]
    other = [jnp.where(core == 0, b, a) for a, b in zip(blocks[::2], blocks[1::2])]
    return jnp.concatenate(mine, axis=1), jnp.concatenate(other, axis=1)


def shards(
    queries,
    latents,
    rope_keys,
    latent_norm_scale,
    key_value_weight,
    out_weight,
    resid,
    ffn_gain,
    expert_ids,
    route_weights,
    gate_weight,
    up_weight,
    down_weight,
):
    tok_rows, local_heads, _ = queries.shape
    groups = lax.axis_size("sp")
    tp_size = lax.axis_size("tp")
    me = lax.axis_index("sp")
    tp_index = lax.axis_index("tp")
    core = tp_index % 2
    width = resid.shape[1]
    columns = width // tp_size
    half_width = width // 2

    positions = (me * tok_rows + jnp.arange(tok_rows, dtype=jnp.int32)).astype(f32)
    cosines, sines = rotary_table(positions, rope_keys.shape[1])
    key_turned = turn_pairs(rope_keys.astype(f32), cosines, sines).astype(bf16)
    normalized_latent = rms_scaled(latents, latent_norm_scale).astype(bf16)
    latent_width = latents.shape[1]
    own_piece = jnp.concatenate([normalized_latent, key_turned], axis=1)
    pieces = [own_piece] + [swap(own_piece, "sp", k) for k in range(1, groups)]

    query_plain = queries[:, :, :PLAIN_WIDTH]
    query_turned = turn_pairs(
        queries[:, :, PLAIN_WIDTH:].astype(f32), cosines[:, None, :], sines[:, None, :]
    ).astype(bf16)

    top_count = expert_ids.shape[1]
    capacity = (3 * tok_rows * top_count + 2 * groups - 1) // (2 * groups)
    slots = groups * capacity
    flat_ids = jnp.transpose(expert_ids).reshape(-1)
    relative = jnp.bitwise_xor(flat_ids, me)
    picked = relative[:, None] == jnp.arange(groups, dtype=jnp.int32)[None, :]
    count = flat_ids.shape[0]
    order = jnp.arange(count, dtype=jnp.int32)
    earlier = (order[:, None] > order[None, :]).astype(bf16)
    ranks = jnp.dot(earlier, picked.astype(bf16), preferred_element_type=f32)
    slot_rank = jnp.sum(jnp.where(picked, ranks, 0.0), axis=1).astype(jnp.int32)
    slot_index = relative * capacity + slot_rank
    chosen = (slot_index[:, None] == jnp.arange(slots, dtype=jnp.int32)[None, :]).astype(bf16)
    send_table = sum(chosen[k * tok_rows : (k + 1) * tok_rows] for k in range(top_count))

    gathered = jnp.concatenate(pieces, axis=0)
    row_count = gathered.shape[0]
    all_latents = gathered[:, :latent_width]
    all_turned = gathered[:, latent_width:]
    per_head = jnp.dot(
        all_latents,
        key_value_weight.reshape(latent_width, -1),
        preferred_element_type=f32,
    ).astype(bf16).reshape(row_count, local_heads, -1)
    key_plain = per_head[:, :, :PLAIN_WIDTH]
    head_values = per_head[:, :, PLAIN_WIDTH:]
    score_scale = queries.shape[-1] ** (-0.5)
    scores = jnp.einsum("qhn,khn->hqk", query_plain, key_plain, preferred_element_type=f32)
    scores = (
        scores + jnp.einsum("qhr,kr->hqk", query_turned, all_turned, preferred_element_type=f32)
    ) * score_scale
    exps = jnp.exp(scores - jnp.max(scores, axis=-1, keepdims=True))
    totals = jnp.sum(exps, axis=-1)
    summed = jnp.einsum("hqk,khv->qhv", exps.astype(bf16), head_values, preferred_element_type=f32)
    attended = (summed / jnp.transpose(totals)[:, :, None]).astype(bf16)
    head_partial = jnp.dot(attended.reshape(tok_rows, -1), out_weight, preferred_element_type=f32)

    mine, other = core_halves(head_partial, columns, core)
    mixed = mine + swap(other.astype(bf16), "tp", 1).astype(f32)
    step = 2
    while step < tp_size:
        rounded = mixed.astype(bf16)
        mixed = rounded.astype(f32) + swap(rounded, "tp", step).astype(f32)
        step *= 2
    resid_half, _ = core_halves(resid, columns, core)
    middle = (resid_half.astype(f32) + mixed).astype(bf16)

    outgoing = lax.dot_general(
        send_table, middle, (((0,), (0,)), ((), ())), preferred_element_type=f32
    ).astype(bf16)
    parts = [outgoing[k * capacity : (k + 1) * capacity] for k in range(groups)]
    arrived = jnp.concatenate(
        [parts[0]] + [swap(parts[k], "sp", k) for k in range(1, groups)], axis=0
    )
    partner = swap(arrived, "tp", 1)
    even = jnp.where(core == 0, arrived, partner)
    odd = jnp.where(core == 0, partner, arrived)
    whole_rows = jnp.concatenate(
        [
            block[:, i : i + columns]
            for i in range(0, half_width, columns)
            for block in (even, odd)
        ],
        axis=1,
    )
    normed = rms_scaled(whole_rows, ffn_gain).astype(bf16)
    gate_act = jnp.dot(normed, gate_weight[0], preferred_element_type=f32)
    up_act = jnp.dot(normed, up_weight[0], preferred_element_type=f32)
    hidden = (jax.nn.silu(gate_act) * up_act).astype(bf16)
    partial_rows = jnp.dot(hidden, down_weight[0], preferred_element_type=f32)

    mine, other = core_halves(partial_rows, columns, core)
    half_rows = (mine + swap(other.astype(bf16), "tp", 1).astype(f32)).astype(bf16)
    parts = [half_rows[k * capacity : (k + 1) * capacity] for k in range(groups)]
    back_rows = jnp.concatenate(
        [parts[0]] + [swap(parts[k], "sp", k) for k in range(1, groups)], axis=0
    )
    chosen_rows = jnp.dot(chosen, back_rows, preferred_element_type=f32)
    routed = sum(
        chosen_rows[k * tok_rows : (k + 1) * tok_rows] * route_weights[:, k : k + 1]
        for k in range(top_count)
    )
    y_index = tp_index // 2
    span = tp_size // 2
    while span > 1:
        span //= 2
        cut = span * columns
        upper = (y_index // span) % 2 == 1
        low, high = routed[:, :cut], routed[:, cut:]
        keep = jnp.where(upper, high, low)
        give = jnp.where(upper, low, high).astype(bf16)
        routed = keep + swap(give, "tp", 2 * span).astype(f32)
    middle_cols = lax.dynamic_slice_in_dim(middle, y_index * columns, columns, 1)
    return (middle_cols.astype(f32) + routed).astype(bf16)


def solution(mesh):
    placed = (
        P("sp", "tp", None),
        P("sp", None),
        P("sp", None),
        P(),
        P(None, "tp", None),
        P("tp", None),
        P("sp", None),
        P(),
        P("sp", None),
        P("sp", None),
        P("sp", None, "tp"),
        P("sp", None, "tp"),
        P("sp", "tp", None),
    )
    return jax.shard_map(
        shards, mesh=mesh, in_specs=placed, out_specs=P("sp", "tp"), check_vma=False
    )
```

```python
import jax
import jax.numpy as jnp
from jax import lax
from jax.experimental import pallas as pl
from jax.experimental.pallas import tpu as pltpu
from jax.sharding import PartitionSpec as P

PLAIN_WIDTH = 128
VALUE_WIDTH = 128

rope_base = 10000.0
norm_eps = 1e-06


f32 = jnp.float32
bf16 = jnp.bfloat16


def rotary_table(positions, width):
    half_width = width // 2
    inverse = rope_base ** (-jnp.arange(half_width, dtype=f32) / half_width)
    turned = positions[:, None] * inverse[None, :]
    return (jnp.cos(turned), jnp.sin(turned))


def turn_pairs(vectors, cosines, sines):
    half_width = vectors.shape[-1] // 2
    front_half = vectors[..., :half_width]
    back_half = vectors[..., half_width:]
    return jnp.concatenate(
        [front_half * cosines - back_half * sines, back_half * cosines + front_half * sines],
        axis=-1,
    )


def rms_scaled(matrix, gain):
    floats = matrix.astype(f32)
    return floats * lax.rsqrt(jnp.mean(floats * floats, axis=-1, keepdims=True) + norm_eps) * gain


def swap(value, axis, distance):
    count = lax.axis_size(axis)
    return lax.ppermute(value, axis, [(i, i ^ distance) for i in range(count)])


def core_halves(matrix, columns, core):
    blocks = [matrix[:, i : i + columns] for i in range(0, matrix.shape[1], columns)]
    mine = [jnp.where(core == 0, a, b) for a, b in zip(blocks[::2], blocks[1::2])]
    other = [jnp.where(core == 0, b, a) for a, b in zip(blocks[::2], blocks[1::2])]
    return jnp.concatenate(mine, axis=1), jnp.concatenate(other, axis=1)


def attention_call(core, query_heads, pieces, key_value_weight, out_weight, columns):
    heads, tok_rows, query_width = query_heads.shape
    latent_width, projected = key_value_weight.shape
    head_width = projected // heads
    value_width = head_width - PLAIN_WIDTH
    count = len(pieces)
    width = out_weight.shape[1]
    score_scale = query_width ** (-0.5)

    def body(core_ref, query_ref, *refs):
        piece_refs = refs[:count]
        kv_hbm, out_hbm, mine_ref, other_ref, kv_vmem, out_vmem, rows_ref, sems = refs[count:]
        kv_copy = pltpu.make_async_copy(kv_hbm, kv_vmem, sems.at[0])
        out_copy = pltpu.make_async_copy(out_hbm, out_vmem, sems.at[1])
        kv_copy.start()
        out_copy.start()
        for i, piece in enumerate(piece_refs):
            rows_ref[i * tok_rows : (i + 1) * tok_rows, :] = piece[...]
        kv_copy.wait()
        latents = rows_ref[:, :latent_width]
        turned = rows_ref[:, latent_width:]
        contract = (((1,), (1,)), ((), ()))
        attended = []
        for h in range(heads):
            weight = kv_vmem[:, h * head_width : (h + 1) * head_width]
            head_kv = jnp.dot(latents, weight, preferred_element_type=f32).astype(bf16)
            query = query_ref[h]
            scores = lax.dot_general(
                query[:, :PLAIN_WIDTH], head_kv[:, :PLAIN_WIDTH], contract, preferred_element_type=f32
            )
            scores = scores + lax.dot_general(
                query[:, PLAIN_WIDTH:], turned, contract, preferred_element_type=f32
            )
            scores = scores * score_scale
            exps = jnp.exp(scores - jnp.max(scores, axis=-1, keepdims=True))
            totals = jnp.sum(exps, axis=-1, keepdims=True)
            summed = jnp.dot(
                exps.astype(bf16), head_kv[:, PLAIN_WIDTH:], preferred_element_type=f32
            )
            attended.append((summed / totals).astype(bf16))
        attended = jnp.concatenate(attended, axis=1)
        out_copy.wait()
        even = core_ref[0] == 0
        for i in range(0, width // columns, 2):
            low = jnp.dot(
                attended, out_vmem[:, i * columns : (i + 1) * columns], preferred_element_type=f32
            )
            high = jnp.dot(
                attended,
                out_vmem[:, (i + 1) * columns : (i + 2) * columns],
                preferred_element_type=f32,
            )
            at = i // 2 * columns
            mine_ref[:, at : at + columns] = jnp.where(even, low, high)
            other_ref[:, at : at + columns] = jnp.where(even, high, low).astype(bf16)

    vmem = pl.BlockSpec(memory_space=pltpu.VMEM)
    hbm = pl.BlockSpec(memory_space=pl.ANY)
    return pl.pallas_call(
        body,
        name="attention",
        out_shape=(
            jax.ShapeDtypeStruct((tok_rows, width // 2), f32),
            jax.ShapeDtypeStruct((tok_rows, width // 2), bf16),
        ),
        in_specs=[pl.BlockSpec(memory_space=pltpu.SMEM), vmem] + [vmem] * count + [hbm, hbm],
        out_specs=(vmem, vmem),
        scratch_shapes=[
            pltpu.VMEM((latent_width, projected), bf16),
            pltpu.VMEM(out_weight.shape, bf16),
            pltpu.VMEM((count * tok_rows, pieces[0].shape[1]), bf16),
            pltpu.SemaphoreType.DMA((2,)),
        ],
        compiler_params=pltpu.CompilerParams(vmem_limit_bytes=16 << 20),
    )(core.reshape(1).astype(jnp.int32), query_heads, *pieces, key_value_weight, out_weight)


def shards(
    queries,
    latents,
    rope_keys,
    latent_norm_scale,
    key_value_weight,
    out_weight,
    resid,
    ffn_gain,
    expert_ids,
    route_weights,
    gate_weight,
    up_weight,
    down_weight,
):
    tok_rows, local_heads, _ = queries.shape
    groups = lax.axis_size("sp")
    tp_size = lax.axis_size("tp")
    me = lax.axis_index("sp")
    tp_index = lax.axis_index("tp")
    core = tp_index % 2
    width = resid.shape[1]
    columns = width // tp_size
    half_width = width // 2

    positions = (me * tok_rows + jnp.arange(tok_rows, dtype=jnp.int32)).astype(f32)
    cosines, sines = rotary_table(positions, rope_keys.shape[1])
    key_turned = turn_pairs(rope_keys.astype(f32), cosines, sines).astype(bf16)
    normalized_latent = rms_scaled(latents, latent_norm_scale).astype(bf16)
    latent_width = latents.shape[1]
    own_piece = jnp.concatenate([normalized_latent, key_turned], axis=1)
    pieces = [own_piece] + [swap(own_piece, "sp", k) for k in range(1, groups)]

    query_plain = queries[:, :, :PLAIN_WIDTH]
    query_turned = turn_pairs(
        queries[:, :, PLAIN_WIDTH:].astype(f32), cosines[:, None, :], sines[:, None, :]
    ).astype(bf16)

    top_count = expert_ids.shape[1]
    capacity = (3 * tok_rows * top_count + 2 * groups - 1) // (2 * groups)
    slots = groups * capacity
    flat_ids = jnp.transpose(expert_ids).reshape(-1)
    relative = jnp.bitwise_xor(flat_ids, me)
    picked = relative[:, None] == jnp.arange(groups, dtype=jnp.int32)[None, :]
    count = flat_ids.shape[0]
    order = jnp.arange(count, dtype=jnp.int32)
    earlier = (order[:, None] > order[None, :]).astype(bf16)
    ranks = jnp.dot(earlier, picked.astype(bf16), preferred_element_type=f32)
    slot_rank = jnp.sum(jnp.where(picked, ranks, 0.0), axis=1).astype(jnp.int32)
    slot_index = relative * capacity + slot_rank
    chosen = (slot_index[:, None] == jnp.arange(slots, dtype=jnp.int32)[None, :]).astype(bf16)
    send_table = sum(chosen[k * tok_rows : (k + 1) * tok_rows] for k in range(top_count))

    query_heads = jnp.transpose(
        jnp.concatenate([query_plain, query_turned], axis=-1), (1, 0, 2)
    )
    mine, other = attention_call(
        core, query_heads, pieces, key_value_weight.reshape(latent_width, -1), out_weight, columns
    )

    mixed = mine + swap(other, "tp", 1).astype(f32)
    step = 2
    while step < tp_size:
        rounded = mixed.astype(bf16)
        mixed = rounded.astype(f32) + swap(rounded, "tp", step).astype(f32)
        step *= 2
    resid_half, _ = core_halves(resid, columns, core)
    middle = (resid_half.astype(f32) + mixed).astype(bf16)

    outgoing = lax.dot_general(
        send_table, middle, (((0,), (0,)), ((), ())), preferred_element_type=f32
    ).astype(bf16)
    parts = [outgoing[k * capacity : (k + 1) * capacity] for k in range(groups)]
    arrived = jnp.concatenate(
        [parts[0]] + [swap(parts[k], "sp", k) for k in range(1, groups)], axis=0
    )
    partner = swap(arrived, "tp", 1)
    even = jnp.where(core == 0, arrived, partner)
    odd = jnp.where(core == 0, partner, arrived)
    whole_rows = jnp.concatenate(
        [
            block[:, i : i + columns]
            for i in range(0, half_width, columns)
            for block in (even, odd)
        ],
        axis=1,
    )
    normed = lax.optimization_barrier(rms_scaled(whole_rows, ffn_gain).astype(bf16))
    gate_act = jnp.dot(normed, gate_weight[0], preferred_element_type=f32)
    up_act = jnp.dot(normed, up_weight[0], preferred_element_type=f32)
    hidden = lax.optimization_barrier((jax.nn.silu(gate_act) * up_act).astype(bf16))
    partial_rows = lax.optimization_barrier(
        jnp.dot(hidden, down_weight[0], preferred_element_type=f32).astype(bf16)
    )

    mine, other = core_halves(partial_rows, columns, core)
    half_rows = (mine.astype(f32) + swap(other, "tp", 1).astype(f32)).astype(bf16)
    parts = [half_rows[k * capacity : (k + 1) * capacity] for k in range(groups)]
    back_rows = jnp.concatenate(
        [parts[0]] + [swap(parts[k], "sp", k) for k in range(1, groups)], axis=0
    )
    chosen_rows = jnp.dot(chosen, back_rows, preferred_element_type=f32)
    routed = sum(
        chosen_rows[k * tok_rows : (k + 1) * tok_rows] * route_weights[:, k : k + 1]
        for k in range(top_count)
    )
    y_index = tp_index // 2
    span = tp_size // 2
    while span > 1:
        span //= 2
        cut = span * columns
        upper = (y_index // span) % 2 == 1
        low, high = routed[:, :cut], routed[:, cut:]
        keep = jnp.where(upper, high, low)
        give = jnp.where(upper, low, high).astype(bf16)
        routed = keep + swap(give, "tp", 2 * span).astype(f32)
    middle_cols = lax.dynamic_slice_in_dim(middle, y_index * columns, columns, 1)
    return (middle_cols.astype(f32) + routed).astype(bf16)


def solution(mesh):
    placed = (
        P("sp", "tp", None),
        P("sp", None),
        P("sp", None),
        P(),
        P(None, "tp", None),
        P("tp", None),
        P("sp", None),
        P(),
        P("sp", None),
        P("sp", None),
        P("sp", None, "tp"),
        P("sp", None, "tp"),
        P("sp", "tp", None),
    )
    return jax.shard_map(
        shards, mesh=mesh, in_specs=placed, out_specs=P("sp", "tp"), check_vma=False
    )
```

```python
import jax
import jax.numpy as jnp
from jax import lax
from jax.experimental import pallas as pl
from jax.experimental.pallas import tpu as pltpu
from jax.sharding import PartitionSpec as P

PLAIN_WIDTH = 128
VALUE_WIDTH = 128

rope_base = 10000.0
norm_eps = 1e-06


f32 = jnp.float32
bf16 = jnp.bfloat16


def rotary_table(positions, width):
    half_width = width // 2
    inverse = rope_base ** (-jnp.arange(half_width, dtype=f32) / half_width)
    turned = positions[:, None] * inverse[None, :]
    return (jnp.cos(turned), jnp.sin(turned))


def turn_pairs(vectors, cosines, sines):
    half_width = vectors.shape[-1] // 2
    front_half = vectors[..., :half_width]
    back_half = vectors[..., half_width:]
    return jnp.concatenate(
        [front_half * cosines - back_half * sines, back_half * cosines + front_half * sines],
        axis=-1,
    )


def rms_scaled(matrix, gain):
    floats = matrix.astype(f32)
    return floats * lax.rsqrt(jnp.mean(floats * floats, axis=-1, keepdims=True) + norm_eps) * gain


def swap(value, axis, distance):
    count = lax.axis_size(axis)
    return lax.ppermute(value, axis, [(i, i ^ distance) for i in range(count)])


def core_halves(matrix, columns, core):
    blocks = [matrix[:, i : i + columns] for i in range(0, matrix.shape[1], columns)]
    mine = [jnp.where(core == 0, a, b) for a, b in zip(blocks[::2], blocks[1::2])]
    other = [jnp.where(core == 0, b, a) for a, b in zip(blocks[::2], blocks[1::2])]
    return jnp.concatenate(mine, axis=1), jnp.concatenate(other, axis=1)


def piece_call(latents, rope_keys, gain, cosines, sines):
    tok_rows, latent_width = latents.shape

    def body(latent_ref, rope_ref, gain_ref, cosine_ref, sine_ref, out_ref):
        out_ref[:, :latent_width] = rms_scaled(latent_ref[...], gain_ref[...]).astype(bf16)
        out_ref[:, latent_width:] = turn_pairs(
            rope_ref[...].astype(f32), cosine_ref[...], sine_ref[...]
        ).astype(bf16)

    return pl.pallas_call(
        body,
        name="piece",
        out_shape=jax.ShapeDtypeStruct((tok_rows, latent_width + rope_keys.shape[1]), bf16),
        compiler_params=pltpu.CompilerParams(vmem_limit_bytes=4 << 20),
    )(latents, rope_keys, gain.reshape(1, -1), cosines, sines)


def attention_call(core, query_heads, pieces, key_value_weight, out_weight, columns):
    heads, tok_rows, query_width = query_heads.shape
    latent_width, projected = key_value_weight.shape
    head_width = projected // heads
    value_width = head_width - PLAIN_WIDTH
    count = len(pieces)
    width = out_weight.shape[1]
    score_scale = query_width ** (-0.5)

    def body(core_ref, query_ref, *refs):
        piece_refs = refs[:count]
        kv_hbm, out_hbm, mine_ref, other_ref, kv_vmem, out_vmem, rows_ref, sems = refs[count:]
        kv_copy = pltpu.make_async_copy(kv_hbm, kv_vmem, sems.at[0])
        out_copy = pltpu.make_async_copy(out_hbm, out_vmem, sems.at[1])
        kv_copy.start()
        out_copy.start()
        for i, piece in enumerate(piece_refs):
            rows_ref[i * tok_rows : (i + 1) * tok_rows, :] = piece[...]
        kv_copy.wait()
        latents = rows_ref[:, :latent_width]
        turned = rows_ref[:, latent_width:]
        contract = (((1,), (1,)), ((), ()))
        attended = []
        for h in range(heads):
            weight = kv_vmem[:, h * head_width : (h + 1) * head_width]
            head_kv = jnp.dot(latents, weight, preferred_element_type=f32).astype(bf16)
            query = query_ref[h]
            scores = lax.dot_general(
                query[:, :PLAIN_WIDTH], head_kv[:, :PLAIN_WIDTH], contract, preferred_element_type=f32
            )
            scores = scores + lax.dot_general(
                query[:, PLAIN_WIDTH:], turned, contract, preferred_element_type=f32
            )
            scores = scores * score_scale
            exps = jnp.exp(scores - jnp.max(scores, axis=-1, keepdims=True))
            totals = jnp.sum(exps, axis=-1, keepdims=True)
            summed = jnp.dot(
                exps.astype(bf16), head_kv[:, PLAIN_WIDTH:], preferred_element_type=f32
            )
            attended.append((summed / totals).astype(bf16))
        attended = jnp.concatenate(attended, axis=1)
        out_copy.wait()
        even = core_ref[0] == 0
        for i in range(0, width // columns, 2):
            low = jnp.dot(
                attended, out_vmem[:, i * columns : (i + 1) * columns], preferred_element_type=f32
            )
            high = jnp.dot(
                attended,
                out_vmem[:, (i + 1) * columns : (i + 2) * columns],
                preferred_element_type=f32,
            )
            at = i // 2 * columns
            mine_ref[:, at : at + columns] = jnp.where(even, low, high)
            other_ref[:, at : at + columns] = jnp.where(even, high, low).astype(bf16)

    vmem = pl.BlockSpec(memory_space=pltpu.VMEM)
    hbm = pl.BlockSpec(memory_space=pl.ANY)
    return pl.pallas_call(
        body,
        name="attention",
        out_shape=(
            jax.ShapeDtypeStruct((tok_rows, width // 2), f32),
            jax.ShapeDtypeStruct((tok_rows, width // 2), bf16),
        ),
        in_specs=[pl.BlockSpec(memory_space=pltpu.SMEM), vmem] + [vmem] * count + [hbm, hbm],
        out_specs=(vmem, vmem),
        scratch_shapes=[
            pltpu.VMEM((latent_width, projected), bf16),
            pltpu.VMEM(out_weight.shape, bf16),
            pltpu.VMEM((count * tok_rows, pieces[0].shape[1]), bf16),
            pltpu.SemaphoreType.DMA((2,)),
        ],
        compiler_params=pltpu.CompilerParams(vmem_limit_bytes=16 << 20),
    )(core.reshape(1).astype(jnp.int32), query_heads, *pieces, key_value_weight, out_weight)


def shards(
    queries,
    latents,
    rope_keys,
    latent_norm_scale,
    key_value_weight,
    out_weight,
    resid,
    ffn_gain,
    expert_ids,
    route_weights,
    gate_weight,
    up_weight,
    down_weight,
):
    tok_rows, local_heads, _ = queries.shape
    groups = lax.axis_size("sp")
    tp_size = lax.axis_size("tp")
    me = lax.axis_index("sp")
    tp_index = lax.axis_index("tp")
    core = tp_index % 2
    width = resid.shape[1]
    columns = width // tp_size
    half_width = width // 2

    positions = (me * tok_rows + jnp.arange(tok_rows, dtype=jnp.int32)).astype(f32)
    cosines, sines = rotary_table(positions, rope_keys.shape[1])
    latent_width = latents.shape[1]
    own_piece = piece_call(latents, rope_keys, latent_norm_scale, cosines, sines)
    pieces = [own_piece] + [swap(own_piece, "sp", k) for k in range(1, groups)]

    query_plain = queries[:, :, :PLAIN_WIDTH]
    query_turned = turn_pairs(
        queries[:, :, PLAIN_WIDTH:].astype(f32), cosines[:, None, :], sines[:, None, :]
    ).astype(bf16)

    query_heads = jnp.transpose(
        jnp.concatenate([query_plain, query_turned], axis=-1), (1, 0, 2)
    )
    mine, other = attention_call(
        core, query_heads, pieces, key_value_weight.reshape(latent_width, -1), out_weight, columns
    )

    mine, other, expert_ids, resid = lax.optimization_barrier((mine, other, expert_ids, resid))
    top_count = expert_ids.shape[1]
    capacity = (3 * tok_rows * top_count + 2 * groups - 1) // (2 * groups)
    slots = groups * capacity
    flat_ids = jnp.transpose(expert_ids).reshape(-1)
    relative = jnp.bitwise_xor(flat_ids, me)
    picked = relative[:, None] == jnp.arange(groups, dtype=jnp.int32)[None, :]
    count = flat_ids.shape[0]
    order = jnp.arange(count, dtype=jnp.int32)
    earlier = (order[:, None] > order[None, :]).astype(bf16)
    ranks = jnp.dot(earlier, picked.astype(bf16), preferred_element_type=f32)
    slot_rank = jnp.sum(jnp.where(picked, ranks, 0.0), axis=1).astype(jnp.int32)
    slot_index = relative * capacity + slot_rank
    chosen = (slot_index[:, None] == jnp.arange(slots, dtype=jnp.int32)[None, :]).astype(bf16)
    send_table = sum(chosen[k * tok_rows : (k + 1) * tok_rows] for k in range(top_count))

    mixed = mine + swap(other, "tp", 1).astype(f32)
    step = 2
    while step < tp_size:
        rounded = mixed.astype(bf16)
        mixed = rounded.astype(f32) + swap(rounded, "tp", step).astype(f32)
        step *= 2
    resid_half, _ = core_halves(resid, columns, core)
    middle = (resid_half.astype(f32) + mixed).astype(bf16)

    outgoing = lax.dot_general(
        send_table, middle, (((0,), (0,)), ((), ())), preferred_element_type=f32
    ).astype(bf16)
    parts = [outgoing[k * capacity : (k + 1) * capacity] for k in range(groups)]
    arrived = jnp.concatenate(
        [parts[0]] + [swap(parts[k], "sp", k) for k in range(1, groups)], axis=0
    )
    partner = swap(arrived, "tp", 1)
    even = jnp.where(core == 0, arrived, partner)
    odd = jnp.where(core == 0, partner, arrived)
    whole_rows = jnp.concatenate(
        [
            block[:, i : i + columns]
            for i in range(0, half_width, columns)
            for block in (even, odd)
        ],
        axis=1,
    )
    normed = lax.optimization_barrier(rms_scaled(whole_rows, ffn_gain).astype(bf16))
    gate_act = jnp.dot(normed, gate_weight[0], preferred_element_type=f32)
    up_act = jnp.dot(normed, up_weight[0], preferred_element_type=f32)
    hidden = lax.optimization_barrier((jax.nn.silu(gate_act) * up_act).astype(bf16))
    partial_rows = lax.optimization_barrier(
        jnp.dot(hidden, down_weight[0], preferred_element_type=f32).astype(bf16)
    )

    mine, other = core_halves(partial_rows, columns, core)
    half_rows = (mine.astype(f32) + swap(other, "tp", 1).astype(f32)).astype(bf16)
    parts = [half_rows[k * capacity : (k + 1) * capacity] for k in range(groups)]
    back_rows = jnp.concatenate(
        [parts[0]] + [swap(parts[k], "sp", k) for k in range(1, groups)], axis=0
    )
    chosen_rows = jnp.dot(chosen, back_rows, preferred_element_type=f32)
    routed = sum(
        chosen_rows[k * tok_rows : (k + 1) * tok_rows] * route_weights[:, k : k + 1]
        for k in range(top_count)
    )
    y_index = tp_index // 2
    span = tp_size // 2
    while span > 1:
        span //= 2
        cut = span * columns
        upper = (y_index // span) % 2 == 1
        low, high = routed[:, :cut], routed[:, cut:]
        keep = jnp.where(upper, high, low)
        give = jnp.where(upper, low, high).astype(bf16)
        routed = keep + swap(give, "tp", 2 * span).astype(f32)
    middle_cols = lax.dynamic_slice_in_dim(middle, y_index * columns, columns, 1)
    return (middle_cols.astype(f32) + routed).astype(bf16)


def solution(mesh):
    placed = (
        P("sp", "tp", None),
        P("sp", None),
        P("sp", None),
        P(),
        P(None, "tp", None),
        P("tp", None),
        P("sp", None),
        P(),
        P("sp", None),
        P("sp", None),
        P("sp", None, "tp"),
        P("sp", None, "tp"),
        P("sp", "tp", None),
    )
    return jax.shard_map(
        shards, mesh=mesh, in_specs=placed, out_specs=P("sp", "tp"), check_vma=False
    )
```
